32 devices in a mesh: sp: 4 (over y, x), dp: 8 (over z, core).
Axes of the slice: x: 2, y: 2, z: 4, core: 2. Of those that a mesh axis runs over, the one named last changes fastest.
Arguments:
- tokens: bfloat16 [8, 512, 2048], P('dp', 'sp'), may hold values from -6 to 6
- query_weight: bfloat16 [2048, 1024], P('dp'), may hold values from -0.125 to 0.125
- key_weight: bfloat16 [2048, 1024], P('dp'), may hold values from -0.125 to 0.125
- value_weight: bfloat16 [2048, 2048], P('dp'), may hold values from -0.125 to 0.125
- output_weight: bfloat16 [2048, 2048], P('dp'), may hold values from -0.125 to 0.125
- log_decay: float32 [2, 16], P(None, 'sp'), may hold values from -0.04 to 0, as said below
Outputs:
- mixed: bfloat16 [8, 512, 2048], P('dp', 'sp')
The draws below stay inside these ranges and needn't reach their ends.
Inputs may be any that keep to these rules, and one draw needn't show every extreme that they name: `log_decay`: every entry is negative: the logarithm of a head's decay per position.
All inputs are finite; a program needn't handle non-finite values.
Results may differ from the reference program's by a relative error of at most 0.012.
Values may be sent and summed in bfloat16 or wider, within the bound.
A program may use at most 128 MiB of HBM per device.

```python
import jax
import jax.numpy as jnp
from jax import lax

D = 2048
HEADS = 16
DK = 64
DV = 128
BLOCK = 512
SEQ = 512
SEQS = 8


def draw_log_decay(key, part):
    first_key, second_key, third_key = jax.random.split(jax.random.fold_in(key, 17), 3)
    share = 0.5
    fast = jax.random.uniform(first_key, (2, HEADS), jnp.float32) < share
    fast_rate = jnp.exp(jax.random.uniform(second_key, (2, HEADS), jnp.float32, jnp.log(1.0 / 80.0), jnp.log(1.0 / 25.0)))
    slow_rate = jax.random.uniform(third_key, (2, HEADS), jnp.float32, 0.3, 2.0) / SEQ
    return (-jnp.where(fast, fast_rate, slow_rate)).astype(jnp.float32)


def level_of(rng, dims, shards, smallest, largest):
    factor_of, own = 1.0, jax.random.fold_in(rng, 6)
    for axis_at, shards_of in shards:
        draws = jnp.exp(jax.random.uniform(jax.random.fold_in(own, axis_at), (shards_of,), jnp.float32, smallest / len(shards), largest / len(shards)))
        factor_of = factor_of * jnp.repeat(draws, dims[axis_at] // shards_of).reshape([-1 if axis == axis_at else 1 for axis in range(len(dims))])
    return factor_of


def gaussian(key, extent, deviation, bound, cuts=(), kind=jnp.bfloat16):
    values = deviation * jax.random.normal(key, extent, jnp.float32)
    if cuts:
        values = values * level_of(key, extent, cuts, -0.22, 0.18)
    return jnp.clip(values, -bound, bound).astype(kind)


def setup_inputs(seed: int = 0) -> dict:
    splits = jax.random.split(jax.random.key(seed), 7)
    return {
        "tokens": gaussian(splits[0], (SEQS, SEQ, D), 1.0, 6.0, ((0, 8), (1, 4))),
        "query_weight": gaussian(splits[1], (D, HEADS * DK), D ** -0.5, 0.125, ((0, 8),)),
        "key_weight": gaussian(splits[2], (D, HEADS * DK), D ** -0.5, 0.125, ((0, 8),)),
        "value_weight": gaussian(splits[3], (D, HEADS * DV), D ** -0.5, 0.125, ((0, 8),)),
        "output_weight": gaussian(splits[4], (HEADS * DV, D), (HEADS * DV) ** -0.5, 0.125, ((0, 8),)),
        "log_decay": draw_log_decay(jax.random.fold_in(splits[6], 71), 0),
    }


exact_precision = lax.Precision.HIGHEST

def rotate(values_part, positions):
    half_dim = values_part.shape[-1] // 2
    frequency = 10000.0 ** (-jnp.arange(half_dim, dtype=jnp.float32) / half_dim)
    angles = positions[:, None] * frequency[None, :]
    cosine = jnp.cos(angles)[:, None, :]
    sine_part = jnp.sin(angles)[:, None, :]
    first = values_part[..., :half_dim]
    second = values_part[..., half_dim:]
    return jnp.concatenate([first * cosine - second * sine_part, first * sine_part + second * cosine], axis=-1)

def retain(query, key_rows, value_rows, log_rate):
    length, heads, key_dim = query.shape
    value_dim = value_rows.shape[-1]
    count = length // BLOCK
    offsets = jnp.arange(BLOCK, dtype=jnp.float32)
    distance = offsets[:, None] - offsets[None, :]
    decay_inner = jnp.where(distance[None] >= 0.0, jnp.exp(log_rate[:, None, None] * jnp.maximum(distance, 0.0)[None]), 0.0)
    decay_query = jnp.exp((offsets[:, None] + 1.0) * log_rate[None, :])[:, :, None]
    decay_key = jnp.exp((BLOCK - 1.0 - offsets)[:, None] * log_rate[None, :])[:, :, None]
    decay_block = jnp.exp(BLOCK * log_rate)[:, None, None]

    def blocks(array):
        return array.reshape(count, BLOCK, heads, array.shape[-1])

    def advance(state, inputs):
        query_block, key_block, value_block = inputs
        query_wide = query_block.astype(jnp.float32)
        key_wide = key_block.astype(jnp.float32)
        value_wide = value_block.astype(jnp.float32)
        inner = jnp.einsum('ihd,jhd->hij', query_wide, key_wide, precision=exact_precision) * decay_inner
        inner = inner.astype(jnp.bfloat16).astype(jnp.float32)
        result = jnp.einsum('hij,jhv->ihv', inner, value_wide, precision=exact_precision)
        result = result + jnp.einsum('ihd,hdv->ihv', query_wide * decay_query, state, precision=exact_precision)
        state = state * decay_block + jnp.einsum('jhd,jhv->hdv', key_wide * decay_key, value_wide, precision=exact_precision)
        return (state, result)
    initial = jnp.zeros((heads, key_dim, value_dim), jnp.float32)
    final_state, outputs = lax.scan(advance, initial, (blocks(query), blocks(key_rows), blocks(value_rows)))
    return outputs.reshape(length, heads, value_dim)

def mechanism(stacked, log_decay):
    length = stacked.shape[0]
    widened = stacked[..., :2 * DK].astype(jnp.float32)
    positions = jnp.arange(length, dtype=jnp.float32)
    query = rotate(widened[..., :DK], positions).astype(jnp.bfloat16)
    key_rows = rotate(widened[..., DK:2 * DK], positions).astype(jnp.bfloat16)
    value_rows = stacked[..., 2 * DK:]
    forward = retain(query, key_rows, value_rows, log_decay[0])
    backward = retain(jnp.flip(query, 0), jnp.flip(key_rows, 0), jnp.flip(value_rows, 0), log_decay[1])
    combined = forward + jnp.flip(backward, 0)
    average = lax.optimization_barrier(jnp.mean(combined, axis=-1, keepdims=True))
    centred = combined - average
    variance = lax.optimization_barrier(jnp.mean(centred * centred, axis=-1, keepdims=True))
    return (centred * lax.rsqrt(variance + 1e-06)).astype(jnp.bfloat16)

def reference(tokens, query_weight, key_weight, value_weight, output_weight, log_decay):

    def one_sequence(rows):
        length = rows.shape[0]
        query = jnp.dot(rows, query_weight, preferred_element_type=jnp.float32).astype(jnp.bfloat16).reshape(length, HEADS, DK)
        key_rows = jnp.dot(rows, key_weight, preferred_element_type=jnp.float32).astype(jnp.bfloat16).reshape(length, HEADS, DK)
        value_rows = jnp.dot(rows, value_weight, preferred_element_type=jnp.float32).astype(jnp.bfloat16).reshape(length, HEADS, DV)
        stacked = jnp.concatenate([query, key_rows, value_rows], axis=2)
        normed = mechanism(stacked, log_decay).reshape(length, HEADS * DV)
        return jnp.dot(normed, output_weight, preferred_element_type=jnp.float32).astype(jnp.bfloat16)
    return lax.map(one_sequence, tokens)
```

```python
import functools

import numpy as np
import jax
import jax.numpy as jnp
from jax import lax
from jax.experimental import pallas as pl
from jax.experimental.pallas import tpu as pltpu
from jax.sharding import PartitionSpec as P

HEADS = 16
DK = 64
DV = 128
BLOCK = 512


exact_precision = lax.Precision.HIGHEST


def rotate(values_part, positions):
    half_dim = values_part.shape[-1] // 2
    frequency = 10000.0 ** (-jnp.arange(half_dim, dtype=jnp.float32) / half_dim)
    angles = positions[:, None] * frequency[None, :]
    cosine = jnp.cos(angles)[:, None, :]
    sine_part = jnp.sin(angles)[:, None, :]
    first = values_part[..., :half_dim]
    second = values_part[..., half_dim:]
    return jnp.concatenate(
        [first * cosine - second * sine_part, first * sine_part + second * cosine], axis=-1
    )


def retain(query, key_rows, value_rows, log_rate):
    length, heads, key_dim = query.shape
    value_dim = value_rows.shape[-1]
    count = length // BLOCK
    offsets = jnp.arange(BLOCK, dtype=jnp.float32)
    distance = offsets[:, None] - offsets[None, :]
    decay_inner = jnp.where(
        distance[None] >= 0.0,
        jnp.exp(log_rate[:, None, None] * jnp.maximum(distance, 0.0)[None]),
        0.0,
    )
    decay_query = jnp.exp((offsets[:, None] + 1.0) * log_rate[None, :])[:, :, None]
    decay_key = jnp.exp((BLOCK - 1.0 - offsets)[:, None] * log_rate[None, :])[:, :, None]
    decay_block = jnp.exp(BLOCK * log_rate)[:, None, None]

    def blocks(array):
        return array.reshape(count, BLOCK, heads, array.shape[-1])

    def advance(state, inputs):
        query_block, key_block, value_block = inputs
        inner = (
            jnp.einsum("ihd,jhd->hij", query_block, key_block, preferred_element_type=jnp.float32)
            * decay_inner
        )
        result = jnp.einsum(
            "hij,jhv->ihv",
            inner.astype(jnp.bfloat16),
            value_block,
            preferred_element_type=jnp.float32,
        )
        query_wide = query_block.astype(jnp.float32) * decay_query
        result = result + jnp.einsum("ihd,hdv->ihv", query_wide, state, precision=exact_precision)
        key_wide = key_block.astype(jnp.float32) * decay_key
        state = state * decay_block + jnp.einsum(
            "jhd,jhv->hdv", key_wide, value_block.astype(jnp.float32), precision=exact_precision
        )
        return (state, result)

    initial = jnp.zeros((heads, key_dim, value_dim), jnp.float32)
    final_state, outputs = lax.scan(
        advance, initial, (blocks(query), blocks(key_rows), blocks(value_rows))
    )
    return outputs.reshape(length, heads, value_dim)


def mechanism(stacked, log_decay):
    length = stacked.shape[0]
    widened = stacked[..., : 2 * DK].astype(jnp.float32)
    positions = jnp.arange(length, dtype=jnp.float32)
    query = rotate(widened[..., :DK], positions).astype(jnp.bfloat16)
    key_rows = rotate(widened[..., DK : 2 * DK], positions).astype(jnp.bfloat16)
    value_rows = stacked[..., 2 * DK :]
    forward = retain(query, key_rows, value_rows, log_decay[0])
    backward = retain(
        jnp.flip(query, 0), jnp.flip(key_rows, 0), jnp.flip(value_rows, 0), log_decay[1]
    )
    combined = forward + jnp.flip(backward, 0)
    average = jnp.mean(combined, axis=-1, keepdims=True)
    centred = combined - average
    variance = jnp.mean(centred * centred, axis=-1, keepdims=True)
    return (centred * lax.rsqrt(variance + 1e-06)).astype(jnp.bfloat16)


def shards(tokens, query_weight, key_weight, value_weight, output_weight, log_decay):
    rows = tokens[0]
    row_count = rows.shape[0]
    local_heads = log_decay.shape[1]
    first_head = lax.axis_index("sp") * local_heads
    own_slices = jnp.concatenate(
        [
            lax.dynamic_slice_in_dim(query_weight, first_head * DK, local_heads * DK, 1),
            lax.dynamic_slice_in_dim(key_weight, first_head * DK, local_heads * DK, 1),
            lax.dynamic_slice_in_dim(value_weight, first_head * DV, local_heads * DV, 1),
        ],
        axis=1,
    )
    own_whole = lax.all_gather(own_slices, "dp", axis=0, tiled=True)
    piece = lax.all_gather(rows, "sp", axis=0, tiled=True)
    count = piece.shape[0]
    product = jnp.dot(piece, own_whole, preferred_element_type=jnp.float32).astype(jnp.bfloat16)
    query_part = product[:, : local_heads * DK].reshape(count, local_heads, DK)
    key_part = product[:, local_heads * DK : 2 * local_heads * DK].reshape(count, local_heads, DK)
    value_part = product[:, 2 * local_heads * DK :].reshape(count, local_heads, DV)
    gathered = jnp.concatenate([query_part, key_part, value_part], axis=2)
    normed = mechanism(gathered, log_decay)
    by_token = lax.all_to_all(normed, "sp", split_axis=0, concat_axis=1, tiled=True).reshape(
        row_count, HEADS * DV
    )
    mixed = jnp.dot(
        by_token,
        lax.all_gather(output_weight, "dp", axis=0, tiled=True),
        preferred_element_type=jnp.float32,
    )
    return mixed.astype(jnp.bfloat16)[None]


MESH = pl.DeviceIdType.MESH
CORES = 2
PIECES = 2


def tables(length):
    half = DK // 2
    frequency = (10000.0 ** (-np.arange(half) / half)).astype(np.float32)
    angles = (np.arange(length, dtype=np.float32)[:, None] * frequency[None, :]).astype(np.float64)
    cosine = np.tile(np.cos(angles), (1, 4)).astype(np.float32)
    sine = np.tile(np.sin(angles), (1, 4)).astype(np.float32)
    swap = np.zeros((2 * DK, 2 * DK), np.float32)
    for lane in range(2 * DK):
        if lane % DK < half:
            swap[lane + half, lane] = -1.0
        else:
            swap[lane - half, lane] = 1.0
    return jnp.asarray(cosine), jnp.asarray(sine), jnp.asarray(swap, jnp.bfloat16)


def layer_kernel(
    S, Z, rate_ref, cos_ref, sin_ref, swap_ref, x_ref, wq_ref, wk_ref, wv_ref, wo_ref, out_ref,
    tok, wqkv, wo, acc, decay, qk, val, nsend, nrm, oacc,
    lsem, tS, tR, qS, qR, qpS, qpR, oS, oR, iS, iR, dS, dR, opS, opR, nS, nR,
):
    s = lax.axis_index("sp")
    d = lax.axis_index("dp")
    z, c = d // CORES, d % CORES
    rows, model = x_ref.shape
    length = S * rows
    depth = wq_ref.shape[0]
    heads = rate_ref.shape[1]
    qc, vc = heads * DK, heads * DV
    oc = wo.shape[3]
    step_rows = depth // PIECES
    sx = s + 1 - 2 * (s % 2)
    sy = (s + 2) % 4
    sd = (sx + 2) % 4
    partner = {"dp": z * CORES + 1 - c}

    def remote(src, send, recv, device, dst=None):
        return pltpu.make_async_remote_copy(
            src_ref=src, dst_ref=src if dst is None else dst, send_sem=send, recv_sem=recv,
            device_id=device, device_id_type=MESH,
        )

    local = [
        pltpu.make_async_copy(wq_ref.at[:, pl.ds(pl.multiple_of(s * qc, qc), qc)], wqkv.at[d, :, pl.ds(0, qc)], lsem.at[0]),
        pltpu.make_async_copy(wk_ref.at[:, pl.ds(pl.multiple_of(s * qc, qc), qc)], wqkv.at[d, :, pl.ds(qc, qc)], lsem.at[1]),
        pltpu.make_async_copy(wv_ref.at[:, pl.ds(pl.multiple_of(s * vc, vc), vc)], wqkv.at[d, :, pl.ds(2 * qc, vc)], lsem.at[2]),
        pltpu.make_async_copy(x_ref, tok.at[s], lsem.at[3]),
    ] + [
        pltpu.make_async_copy(wo_ref.at[:, pl.ds(j * oc, oc)], wo.at[d, j], lsem.at[4 + j]) for j in range(S)
    ]
    for copy in local:
        copy.start()

    barrier = pltpu.get_barrier_semaphore()

    def greet(device):
        pl.semaphore_signal(barrier, inc=1, device_id=device, device_id_type=MESH)

    for other in range(1, S):
        greet({"sp": (s + other) % S})
    greet(partner)
    pl.when(z > 0)(lambda: greet({"dp": d - CORES}))
    pl.when(z < Z - 1)(lambda: greet({"dp": d + CORES}))
    inside = (z > 0) & (z < Z - 1)
    pl.when(inside)(lambda: pl.semaphore_wait(barrier, S + 2))
    pl.when(jnp.logical_not(inside))(lambda: pl.semaphore_wait(barrier, S + min(Z - 1, 1)))

    def side(way):
        return {"dp": d + CORES if way == 0 else d - CORES}

    def has_side(way):
        return z < Z - 1 if way == 0 else z > 0

    def q_copy(way, src, piece, to=None):
        ref = wqkv.at[src * CORES + c, pl.ds(piece * step_rows, step_rows)]
        return remote(ref, qS.at[way, src, piece], qR.at[src, piece], side(way if to is None else to))

    def o_piece(block, quarter, piece):
        return wo.at[block, quarter, pl.ds(piece * step_rows, step_rows)]

    def o_copy(way, src, piece, to=None):
        return remote(o_piece(src * CORES + c, s, piece), oS.at[way, src, piece], oR.at[src, piece], side(way if to is None else to))

    def qp_copy(src, mine=True):
        ref = wqkv.at[src * CORES + (c if mine else 1 - c)]
        return remote(ref, qpS.at[src], qpR.at[src], partner)

    def op_copy(src, mine=True):
        ref = wo.at[src * CORES + (c if mine else 1 - c)]
        return remote(ref, opS.at[src], opR.at[src], partner)

    def i_copy(axis, src, piece, mine=True):
        to = sx if axis == 0 else sy
        return remote(o_piece(src * CORES + c, s if mine else to, piece), iS.at[axis, src, piece], iR.at[axis, src, piece], {"sp": to})

    def d_copy(src, piece, mine=True):
        first = piece < PIECES // 2
        to = sy if first else sx
        quarter = (sx if first else sy) if mine else sd
        return remote(o_piece(src * CORES + c, quarter, piece), dS.at[src, piece], dR.at[src, piece], {"sp": to})

    def t_copy(other):
        to = (s + other) % S
        return remote(tok.at[s], tS.at[other], tR.at[other], {"sp": to})

    def t_wait(other):
        frm = (s + S - other) % S
        remote(tok.at[frm], tS.at[other], tR.at[other], {"sp": frm}).wait_recv()

    def n_copy(head, j):
        return remote(
            nsend.at[head, j], nS.at[head, j], nR.at[head, s], {"sp": j},
            dst=nrm.at[s, :, pl.ds(head * DV, DV)],
        )

    def n_wait(head, j):
        remote(nsend.at[head, j], nS.at[head, j], nR.at[head, j], {"sp": j}, dst=nrm.at[j, :, pl.ds(head * DV, DV)]).wait_recv()

    def each(count, fn):
        for piece in range(count):
            fn(piece)

    def own_o(way):
        each(PIECES, lambda piece: o_copy(way, z, piece).start())

    for copy in local[:3]:
        copy.wait()
    for way in (0, 1):
        pl.when(has_side(way))(lambda way=way: each(PIECES, lambda piece: q_copy(way, z, piece).start()))
    local[3].wait()
    for other in range(1, S):
        t_copy(other).start()
    qp_copy(z).start()
    for copy in local[4:]:
        copy.wait()
    op_copy(z).start()
    pl.when(z == 0)(lambda: own_o(0))
    pl.when(z == Z - 1)(lambda: own_o(1))

    for head in range(heads):
        fast, slow = rate_ref[0, head], rate_ref[1, head]

        @pl.loop(0, S)
        def _(j):
            at = lax.broadcasted_iota(jnp.int32, (rows, length), 0) + j * rows
            gap = (at - lax.broadcasted_iota(jnp.int32, (rows, length), 1)).astype(jnp.float32)
            weight = jnp.exp(jnp.where(gap >= 0.0, gap * fast, gap * (-slow)))
            decay[head, pl.ds(pl.multiple_of(j * rows, rows), rows), :] = jnp.where(gap == 0.0, 2.0, weight)

    width = 2 * qc + vc
    tile = 256

    def project(src, first):
        qp_copy(src, mine=False).wait_recv()
        wide = CORES * depth
        cols = pl.ds(pl.multiple_of(src * wide, wide), wide)

        @pl.loop(0, width // tile)
        def _(n):
            at = pl.ds(pl.multiple_of(n * tile, tile), tile)
            part = jnp.dot(
                tok[:, :, cols].reshape(length, wide),
                wqkv[pl.ds(src * CORES, CORES), :, at].reshape(wide, tile),
                preferred_element_type=jnp.float32,
            )
            if first:
                acc[:, at] = part
            else:
                acc[:, at] += part

    for other in range(1, S):
        t_wait(other)
    project(z, True)

    def sources(k):
        return ((0, z - k, z - k >= 0), (1, z + k, z + k < Z))

    for k in range(1, Z):
        for way, src, there in sources(k):
            @pl.when(there)
            def _():
                for piece in range(PIECES):
                    q_copy(way, src, piece, 1 - way).wait_recv()
                    pl.when(has_side(way))(lambda: q_copy(way, src, piece).start())
                qp_copy(src).start()
        if k < Z - 1:
            pl.when(z == k)(lambda: own_o(0))
            pl.when(z == Z - 1 - k)(lambda: own_o(1))
        for way, src, there in sources(k):
            pl.when(there)(lambda: project(src, False))

    for pair in range(qc // (2 * DK)):
        for part in range(2):
            at = pl.ds(part * qc + pair * 2 * DK, 2 * DK)
            flat = acc[:, at].astype(jnp.bfloat16)
            turned = jnp.dot(flat, swap_ref[...], preferred_element_type=jnp.float32)
            qk[:, at] = (flat.astype(jnp.float32) * cos_ref[...] + turned * sin_ref[...]).astype(jnp.bfloat16)
    val[...] = acc[:, 2 * qc :].astype(jnp.bfloat16)

    def retain_head(head):
        pair = head // 2
        lane = lax.broadcasted_iota(jnp.int32, (rows, 2 * DK), 1)
        mine = (lane // DK) == (head % 2)
        for j in range(S):
            here = slice(j * rows, (j + 1) * rows)
            query = qk[here, pair * 2 * DK : (pair + 1) * 2 * DK]
            query = jnp.where(mine, query.astype(jnp.float32), 0.0).astype(jnp.bfloat16)
            scores = lax.dot_general(
                query, qk[:, qc + pair * 2 * DK : qc + (pair + 1) * 2 * DK],
                (((1,), (1,)), ((), ())), preferred_element_type=jnp.float32,
            )
            scores = (scores * decay[head, here, :]).astype(jnp.bfloat16)
            ret = jnp.dot(scores, val[:, head * DV : (head + 1) * DV], preferred_element_type=jnp.float32)
            centred = ret - jnp.mean(ret, axis=-1, keepdims=True)
            variance = jnp.mean(centred * centred, axis=-1, keepdims=True)
            normed = (centred * lax.rsqrt(variance + 1e-06)).astype(jnp.bfloat16)
            nsend[head, j] = normed

            @pl.when(j == s)
            def _():
                nrm[s, :, head * DV : (head + 1) * DV] = normed

            @pl.when(j != s)
            def _():
                n_copy(head, j).start()

    def o_step(k):
        for way, src, there in sources(k):
            @pl.when(there)
            def _():
                for piece in range(PIECES):
                    o_copy(way, src, piece, 1 - way).wait_recv()
                    pl.when(has_side(way))(lambda: o_copy(way, src, piece).start())
                    i_copy(0, src, piece).start()
                    i_copy(1, src, piece).start()

    def o_relay(k):
        for way, src, there in sources(k):
            @pl.when(there)
            def _():
                for piece in range(PIECES):
                    i_copy(0, src, piece, mine=False).wait_recv()
                    i_copy(1, src, piece, mine=False).wait_recv()
                    d_copy(src, piece).start()

    def o_share(k):
        for way, src, there in sources(k):
            @pl.when(there)
            def _():
                for piece in range(PIECES):
                    d_copy(src, piece, mine=False).wait_recv()
                op_copy(src).start()

    def finish(src, first):
        op_copy(src, mine=False).wait_recv()

        @pl.loop(0, S)
        def _(j):
            at = pl.ds(pl.multiple_of(j * oc, oc), oc)
            part = jnp.dot(
                nrm[src], wo[pl.ds(src * CORES, CORES), j].reshape(CORES * depth, oc),
                preferred_element_type=jnp.float32,
            )
            if first:
                oacc[:, at] = part
            else:
                oacc[:, at] += part

    for head in range(heads):
        retain_head(head)
        if head == heads - 2:
            o_step(1)
    o_step(2)
    o_relay(1)
    for j in range(S):
        @pl.when(j != s)
        def _():
            for head in range(heads):
                n_wait(head, j)
    finish(z, True)
    o_share(1)
    o_step(3)
    o_relay(2)
    for way, src, there in sources(1):
        pl.when(there)(lambda: finish(src, False))
    o_share(2)
    o_relay(3)
    for way, src, there in sources(2):
        pl.when(there)(lambda: finish(src, False))
    o_share(3)
    for way, src, there in sources(3):
        pl.when(there)(lambda: finish(src, False))
    out_ref[...] = oacc[...].astype(out_ref.dtype)

    for other in range(1, S):
        t_copy(other).wait_send()
    for way in (0, 1):
        @pl.when(has_side(way))
        def _():
            for piece in range(PIECES):
                q_copy(way, z, piece).wait_send()
                o_copy(way, z, piece).wait_send()
    qp_copy(z).wait_send()
    op_copy(z).wait_send()
    for k in range(1, Z):
        for way, src, there in sources(k):
            @pl.when(there)
            def _():
                qp_copy(src).wait_send()
                op_copy(src).wait_send()
                for piece in range(PIECES):
                    i_copy(0, src, piece).wait_send()
                    i_copy(1, src, piece).wait_send()
                    d_copy(src, piece).wait_send()

            @pl.when(there & has_side(way))
            def _():
                for piece in range(PIECES):
                    q_copy(way, src, piece).wait_send()
                    o_copy(way, src, piece).wait_send()
    for head in range(heads):
        for j in range(S):
            pl.when(j != s)(lambda: n_copy(head, j).wait_send())


def fused(S, Z, tokens, query_weight, key_weight, value_weight, output_weight, log_decay):
    rows, model = tokens.shape[1:]
    depth = query_weight.shape[0]
    heads = log_decay.shape[1]
    length = S * rows
    width = heads * (2 * DK + DV)
    oc = output_weight.shape[1] // S
    cosine, sine, swap = tables(length)
    vmem, anyplace = pl.BlockSpec(memory_space=pltpu.VMEM), pl.BlockSpec(memory_space=pl.ANY)
    dma = pltpu.SemaphoreType.DMA
    bf, f32 = jnp.bfloat16, jnp.float32
    out = pl.pallas_call(
        functools.partial(layer_kernel, S, Z),
        out_shape=jax.ShapeDtypeStruct((rows, output_weight.shape[1]), bf),
        in_specs=[pl.BlockSpec(memory_space=pltpu.SMEM)] + [vmem] * 3 + [anyplace] * 5,
        out_specs=vmem,
        scratch_shapes=[
            pltpu.VMEM((S, rows, model), bf),
            pltpu.VMEM((Z * CORES, depth, width), bf),
            pltpu.VMEM((Z * CORES, S, depth, oc), bf),
            pltpu.VMEM((length, width), f32),
            pltpu.VMEM((heads, length, length), f32),
            pltpu.VMEM((length, 2 * heads * DK), bf),
            pltpu.VMEM((length, heads * DV), bf),
            pltpu.VMEM((heads, S, rows, DV), bf),
            pltpu.VMEM((S, rows, heads * DV), bf),
            pltpu.VMEM((rows, S * oc), f32),
            dma((4 + S,)), dma((S,)), dma((S,)),
            dma((2, Z, PIECES)), dma((Z, PIECES)), dma((Z,)), dma((Z,)),
            dma((2, Z, PIECES)), dma((Z, PIECES)),
            dma((2, Z, PIECES)), dma((2, Z, PIECES)), dma((Z, PIECES)), dma((Z, PIECES)),
            dma((Z,)), dma((Z,)), dma((heads, S)), dma((heads, S)),
        ],
        compiler_params=pltpu.CompilerParams(
            collective_id=0, has_side_effects=True, vmem_limit_bytes=60 * 1024 * 1024
        ),
    )(log_decay, cosine, sine, swap, tokens[0], query_weight, key_weight, value_weight, output_weight)
    return out[None]


def solution(mesh):
    S, D = mesh.shape["sp"], mesh.shape["dp"]
    Z = D // CORES

    def layer(tokens, query_weight, key_weight, value_weight, output_weight, log_decay):
        rows = tokens.shape[1]
        depth = query_weight.shape[0]
        heads = log_decay.shape[1]
        fits = (
            S == 4 and D == CORES * Z and S * rows == BLOCK and (heads * DK) % 256 == 0
            and heads * DV == CORES * depth and rows % 128 == 0
        )
        args = (tokens, query_weight, key_weight, value_weight, output_weight, log_decay)
        return fused(S, Z, *args) if fits else shards(*args)

    placed = (
        P("dp", "sp", None),
        P("dp", None),
        P("dp", None),
        P("dp", None),
        P("dp", None),
        P(None, "sp"),
    )
    return jax.shard_map(
        layer, mesh=mesh, in_specs=placed, out_specs=P("dp", "sp", None), check_vma=False
    )
```

```python
import functools

import numpy as np
import jax
import jax.numpy as jnp
from jax import lax
from jax.experimental import pallas as pl
from jax.experimental.pallas import tpu as pltpu
from jax.sharding import PartitionSpec as P

HEADS = 16
DK = 64
DV = 128
BLOCK = 512


exact_precision = lax.Precision.HIGHEST


def rotate(values_part, positions):
    half_dim = values_part.shape[-1] // 2
    frequency = 10000.0 ** (-jnp.arange(half_dim, dtype=jnp.float32) / half_dim)
    angles = positions[:, None] * frequency[None, :]
    cosine = jnp.cos(angles)[:, None, :]
    sine_part = jnp.sin(angles)[:, None, :]
    first = values_part[..., :half_dim]
    second = values_part[..., half_dim:]
    return jnp.concatenate(
        [first * cosine - second * sine_part, first * sine_part + second * cosine], axis=-1
    )


def retain(query, key_rows, value_rows, log_rate):
    length, heads, key_dim = query.shape
    value_dim = value_rows.shape[-1]
    count = length // BLOCK
    offsets = jnp.arange(BLOCK, dtype=jnp.float32)
    distance = offsets[:, None] - offsets[None, :]
    decay_inner = jnp.where(
        distance[None] >= 0.0,
        jnp.exp(log_rate[:, None, None] * jnp.maximum(distance, 0.0)[None]),
        0.0,
    )
    decay_query = jnp.exp((offsets[:, None] + 1.0) * log_rate[None, :])[:, :, None]
    decay_key = jnp.exp((BLOCK - 1.0 - offsets)[:, None] * log_rate[None, :])[:, :, None]
    decay_block = jnp.exp(BLOCK * log_rate)[:, None, None]

    def blocks(array):
        return array.reshape(count, BLOCK, heads, array.shape[-1])

    def advance(state, inputs):
        query_block, key_block, value_block = inputs
        inner = (
            jnp.einsum("ihd,jhd->hij", query_block, key_block, preferred_element_type=jnp.float32)
            * decay_inner
        )
        result = jnp.einsum(
            "hij,jhv->ihv",
            inner.astype(jnp.bfloat16),
            value_block,
            preferred_element_type=jnp.float32,
        )
        query_wide = query_block.astype(jnp.float32) * decay_query
        result = result + jnp.einsum("ihd,hdv->ihv", query_wide, state, precision=exact_precision)
        key_wide = key_block.astype(jnp.float32) * decay_key
        state = state * decay_block + jnp.einsum(
            "jhd,jhv->hdv", key_wide, value_block.astype(jnp.float32), precision=exact_precision
        )
        return (state, result)

    initial = jnp.zeros((heads, key_dim, value_dim), jnp.float32)
    final_state, outputs = lax.scan(
        advance, initial, (blocks(query), blocks(key_rows), blocks(value_rows))
    )
    return outputs.reshape(length, heads, value_dim)


def mechanism(stacked, log_decay):
    length = stacked.shape[0]
    widened = stacked[..., : 2 * DK].astype(jnp.float32)
    positions = jnp.arange(length, dtype=jnp.float32)
    query = rotate(widened[..., :DK], positions).astype(jnp.bfloat16)
    key_rows = rotate(widened[..., DK : 2 * DK], positions).astype(jnp.bfloat16)
    value_rows = stacked[..., 2 * DK :]
    forward = retain(query, key_rows, value_rows, log_decay[0])
    backward = retain(
        jnp.flip(query, 0), jnp.flip(key_rows, 0), jnp.flip(value_rows, 0), log_decay[1]
    )
    combined = forward + jnp.flip(backward, 0)
    average = jnp.mean(combined, axis=-1, keepdims=True)
    centred = combined - average
    variance = jnp.mean(centred * centred, axis=-1, keepdims=True)
    return (centred * lax.rsqrt(variance + 1e-06)).astype(jnp.bfloat16)


def shards(tokens, query_weight, key_weight, value_weight, output_weight, log_decay):
    rows = tokens[0]
    row_count = rows.shape[0]
    local_heads = log_decay.shape[1]
    first_head = lax.axis_index("sp") * local_heads
    own_slices = jnp.concatenate(
        [
            lax.dynamic_slice_in_dim(query_weight, first_head * DK, local_heads * DK, 1),
            lax.dynamic_slice_in_dim(key_weight, first_head * DK, local_heads * DK, 1),
            lax.dynamic_slice_in_dim(value_weight, first_head * DV, local_heads * DV, 1),
        ],
        axis=1,
    )
    own_whole = lax.all_gather(own_slices, "dp", axis=0, tiled=True)
    piece = lax.all_gather(rows, "sp", axis=0, tiled=True)
    count = piece.shape[0]
    product = jnp.dot(piece, own_whole, preferred_element_type=jnp.float32).astype(jnp.bfloat16)
    query_part = product[:, : local_heads * DK].reshape(count, local_heads, DK)
    key_part = product[:, local_heads * DK : 2 * local_heads * DK].reshape(count, local_heads, DK)
    value_part = product[:, 2 * local_heads * DK :].reshape(count, local_heads, DV)
    gathered = jnp.concatenate([query_part, key_part, value_part], axis=2)
    normed = mechanism(gathered, log_decay)
    by_token = lax.all_to_all(normed, "sp", split_axis=0, concat_axis=1, tiled=True).reshape(
        row_count, HEADS * DV
    )
    mixed = jnp.dot(
        by_token,
        lax.all_gather(output_weight, "dp", axis=0, tiled=True),
        preferred_element_type=jnp.float32,
    )
    return mixed.astype(jnp.bfloat16)[None]


MESH = pl.DeviceIdType.MESH
CORES = 2
PIECES = 2


def tables(length):
    half = DK // 2
    frequency = (10000.0 ** (-np.arange(half) / half)).astype(np.float32)
    angles = (np.arange(length, dtype=np.float32)[:, None] * frequency[None, :]).astype(np.float64)
    cosine = np.tile(np.cos(angles), (1, 4)).astype(np.float32)
    sine = np.tile(np.sin(angles), (1, 4)).astype(np.float32)
    swap = np.zeros((2 * DK, 2 * DK), np.float32)
    for lane in range(2 * DK):
        if lane % DK < half:
            swap[lane + half, lane] = -1.0
        else:
            swap[lane - half, lane] = 1.0
    return jnp.asarray(cosine), jnp.asarray(sine), jnp.asarray(swap, jnp.bfloat16)


def layer_kernel(
    S, Z, rate_ref, cos_ref, sin_ref, swap_ref, x_ref, wq_ref, wk_ref, wv_ref, wo_ref, out_ref,
    tok, wqkv, wo, acc, decay, qk, val, nsend, nrm, oacc,
    lsem, tS, tR, qS, qR, qpS, qpR, oS, oR, iS, iR, dS, dR, opS, opR, nS, nR,
):
    s = lax.axis_index("sp")
    d = lax.axis_index("dp")
    z, c = d // CORES, d % CORES
    rows, model = x_ref.shape
    length = S * rows
    depth = wq_ref.shape[0]
    heads = rate_ref.shape[1]
    qc, vc = heads * DK, heads * DV
    oc = wo.shape[3]
    step_rows = depth // PIECES
    sx = s + 1 - 2 * (s % 2)
    sy = (s + 2) % 4
    sd = (sx + 2) % 4
    partner = {"dp": z * CORES + 1 - c}

    def remote(src, send, recv, device, dst=None):
        return pltpu.make_async_remote_copy(
            src_ref=src, dst_ref=src if dst is None else dst, send_sem=send, recv_sem=recv,
            device_id=device, device_id_type=MESH,
        )

    local = [
        pltpu.make_async_copy(wq_ref.at[:, pl.ds(pl.multiple_of(s * qc, qc), qc)], wqkv.at[d, :, pl.ds(0, qc)], lsem.at[0]),
        pltpu.make_async_copy(wk_ref.at[:, pl.ds(pl.multiple_of(s * qc, qc), qc)], wqkv.at[d, :, pl.ds(qc, qc)], lsem.at[1]),
        pltpu.make_async_copy(wv_ref.at[:, pl.ds(pl.multiple_of(s * vc, vc), vc)], wqkv.at[d, :, pl.ds(2 * qc, vc)], lsem.at[2]),
        pltpu.make_async_copy(x_ref, tok.at[s], lsem.at[3]),
    ] + [
        pltpu.make_async_copy(wo_ref.at[:, pl.ds(j * oc, oc)], wo.at[d, j], lsem.at[4 + j]) for j in range(S)
    ]
    for copy in local:
        copy.start()

    barrier = pltpu.get_barrier_semaphore()

    def greet(device):
        pl.semaphore_signal(barrier, inc=1, device_id=device, device_id_type=MESH)

    for other in range(1, S):
        greet({"sp": (s + other) % S})
    greet(partner)
    pl.when(z > 0)(lambda: greet({"dp": d - CORES}))
    pl.when(z < Z - 1)(lambda: greet({"dp": d + CORES}))
    inside = (z > 0) & (z < Z - 1)
    pl.when(inside)(lambda: pl.semaphore_wait(barrier, S + 2))
    pl.when(jnp.logical_not(inside))(lambda: pl.semaphore_wait(barrier, S + min(Z - 1, 1)))

    def side(way):
        return {"dp": d + CORES if way == 0 else d - CORES}

    def has_side(way):
        return z < Z - 1 if way == 0 else z > 0

    def q_copy(way, src, piece, to=None):
        ref = wqkv.at[src * CORES + c, pl.ds(piece * step_rows, step_rows)]
        return remote(ref, qS.at[way, src, piece], qR.at[src, piece], side(way if to is None else to))

    def o_piece(block, quarter, piece):
        return wo.at[block, quarter, pl.ds(piece * step_rows, step_rows)]

    def o_copy(way, src, piece, to=None):
        return remote(o_piece(src * CORES + c, s, piece), oS.at[way, src, piece], oR.at[src, piece], side(way if to is None else to))

    def qp_copy(src, mine=True):
        ref = wqkv.at[src * CORES + (c if mine else 1 - c)]
        return remote(ref, qpS.at[src], qpR.at[src], partner)

    def op_copy(src, mine=True):
        ref = wo.at[src * CORES + (c if mine else 1 - c)]
        return remote(ref, opS.at[src], opR.at[src], partner)

    def i_copy(axis, src, piece, mine=True):
        to = sx if axis == 0 else sy
        return remote(o_piece(src * CORES + c, s if mine else to, piece), iS.at[axis, src, piece], iR.at[axis, src, piece], {"sp": to})

    def d_copy(src, piece, mine=True):
        first = piece < PIECES // 2
        to = sy if first else sx
        quarter = (sx if first else sy) if mine else sd
        return remote(o_piece(src * CORES + c, quarter, piece), dS.at[src, piece], dR.at[src, piece], {"sp": to})

    def t_copy(other):
        to = (s + other) % S
        return remote(tok.at[s], tS.at[other], tR.at[other], {"sp": to})

    def t_wait(other):
        frm = (s + S - other) % S
        remote(tok.at[frm], tS.at[other], tR.at[other], {"sp": frm}).wait_recv()

    def n_copy(head, j):
        return remote(
            nsend.at[head, j], nS.at[head, j], nR.at[head, s], {"sp": j},
            dst=nrm.at[s, :, pl.ds(head * DV, DV)],
        )

    def n_wait(head, j):
        remote(nsend.at[head, j], nS.at[head, j], nR.at[head, j], {"sp": j}, dst=nrm.at[j, :, pl.ds(head * DV, DV)]).wait_recv()

    def each(count, fn):
        for piece in range(count):
            fn(piece)

    def own_o(way):
        each(PIECES, lambda piece: o_copy(way, z, piece).start())

    for copy in local[:3]:
        copy.wait()
    for way in (0, 1):
        pl.when(has_side(way))(lambda way=way: each(PIECES, lambda piece: q_copy(way, z, piece).start()))
    local[3].wait()
    for other in range(1, S):
        t_copy(other).start()
    qp_copy(z).start()
    for copy in local[4:]:
        copy.wait()
    for way in (0, 1):
        pl.when(has_side(way))(lambda way=way: own_o(way))
    op_copy(z).start()

    for head in range(heads):
        fast, slow = rate_ref[0, head], rate_ref[1, head]

        @pl.loop(0, S)
        def _(j):
            at = lax.broadcasted_iota(jnp.int32, (rows, length), 0) + j * rows
            gap = (at - lax.broadcasted_iota(jnp.int32, (rows, length), 1)).astype(jnp.float32)
            weight = jnp.exp(jnp.where(gap >= 0.0, gap * fast, gap * (-slow)))
            decay[head, pl.ds(pl.multiple_of(j * rows, rows), rows), :] = jnp.where(gap == 0.0, 2.0, weight)

    width = 2 * qc + vc
    tile = 256

    def project(src, first):
        qp_copy(src, mine=False).wait_recv()
        wide = CORES * depth
        cols = pl.ds(pl.multiple_of(src * wide, wide), wide)

        @pl.loop(0, width // tile)
        def _(n):
            at = pl.ds(pl.multiple_of(n * tile, tile), tile)
            part = jnp.dot(
                tok[:, :, cols].reshape(length, wide),
                wqkv[pl.ds(src * CORES, CORES), :, at].reshape(wide, tile),
                preferred_element_type=jnp.float32,
            )
            if first:
                acc[:, at] = part
            else:
                acc[:, at] += part

    for other in range(1, S):
        t_wait(other)
    project(z, True)

    def sources(k):
        return ((0, z - k, z - k >= 0), (1, z + k, z + k < Z))

    def q_step(k):
        for way, src, there in sources(k):
            @pl.when(there)
            def _():
                for piece in range(PIECES):
                    q_copy(way, src, piece, 1 - way).wait_recv()
                    pl.when(has_side(way))(lambda: q_copy(way, src, piece).start())
                qp_copy(src).start()

    def o_step(k):
        for way, src, there in sources(k):
            @pl.when(there)
            def _():
                for piece in range(PIECES):
                    o_copy(way, src, piece, 1 - way).wait_recv()
                    pl.when(has_side(way))(lambda: o_copy(way, src, piece).start())
                for piece in range(PIECES):
                    i_copy(0, src, piece).start()
                    i_copy(1, src, PIECES - 1 - piece).start()

    def o_relay(k):
        for way, src, there in sources(k):
            @pl.when(there)
            def _():
                for near in range(PIECES // 2):
                    for axis, piece in ((0, near), (1, PIECES - 1 - near)):
                        i_copy(axis, src, piece, mine=False).wait_recv()
                        d_copy(src, piece).start()

    def o_share(k):
        for way, src, there in sources(k):
            @pl.when(there)
            def _():
                for near in range(PIECES // 2):
                    i_copy(1, src, near, mine=False).wait_recv()
                    i_copy(0, src, PIECES - 1 - near, mine=False).wait_recv()
                for piece in range(PIECES):
                    d_copy(src, piece, mine=False).wait_recv()
                op_copy(src).start()

    def project_step(k):
        for way, src, there in sources(k):
            pl.when(there)(lambda: project(src, False))

    q_step(1)
    o_step(1)
    project_step(1)
    q_step(2)
    o_step(2)
    o_relay(1)
    project_step(2)
    q_step(3)
    project_step(3)

    for pair in range(qc // (2 * DK)):
        for part in range(2):
            at = pl.ds(part * qc + pair * 2 * DK, 2 * DK)
            flat = acc[:, at].astype(jnp.bfloat16)
            turned = jnp.dot(flat, swap_ref[...], preferred_element_type=jnp.float32)
            qk[:, at] = (flat.astype(jnp.float32) * cos_ref[...] + turned * sin_ref[...]).astype(jnp.bfloat16)
    val[...] = acc[:, 2 * qc :].astype(jnp.bfloat16)

    def retain_head(head):
        pair = head // 2
        lane = lax.broadcasted_iota(jnp.int32, (rows, 2 * DK), 1)
        mine = (lane // DK) == (head % 2)
        for j in range(S):
            here = slice(j * rows, (j + 1) * rows)
            query = qk[here, pair * 2 * DK : (pair + 1) * 2 * DK]
            query = jnp.where(mine, query.astype(jnp.float32), 0.0).astype(jnp.bfloat16)
            scores = lax.dot_general(
                query, qk[:, qc + pair * 2 * DK : qc + (pair + 1) * 2 * DK],
                (((1,), (1,)), ((), ())), preferred_element_type=jnp.float32,
            )
            scores = (scores * decay[head, here, :]).astype(jnp.bfloat16)
            ret = jnp.dot(scores, val[:, head * DV : (head + 1) * DV], preferred_element_type=jnp.float32)
            centred = ret - jnp.mean(ret, axis=-1, keepdims=True)
            variance = jnp.mean(centred * centred, axis=-1, keepdims=True)
            normed = (centred * lax.rsqrt(variance + 1e-06)).astype(jnp.bfloat16)
            nsend[head, j] = normed

            @pl.when(j == s)
            def _():
                nrm[s, :, head * DV : (head + 1) * DV] = normed

            @pl.when(j != s)
            def _():
                n_copy(head, j).start()

    def finish(src, first):
        op_copy(src, mine=False).wait_recv()

        @pl.loop(0, S)
        def _(j):
            at = pl.ds(pl.multiple_of(j * oc, oc), oc)
            part = jnp.dot(
                nrm[src], wo[pl.ds(src * CORES, CORES), j].reshape(CORES * depth, oc),
                preferred_element_type=jnp.float32,
            )
            if first:
                oacc[:, at] = part
            else:
                oacc[:, at] += part

    def finish_step(k):
        for way, src, there in sources(k):
            pl.when(there)(lambda: finish(src, False))

    for head in range(heads):
        retain_head(head)
        if head == 0:
            o_relay(2)
        if head == heads - 2:
            o_step(3)
    o_share(1)
    o_relay(3)
    for j in range(S):
        @pl.when(j != s)
        def _():
            for head in range(heads):
                n_wait(head, j)
    finish(z, True)
    finish_step(1)
    o_share(2)
    o_share(3)
    finish_step(2)
    finish_step(3)
    out_ref[...] = oacc[...].astype(out_ref.dtype)

    for other in range(1, S):
        t_copy(other).wait_send()
    for way in (0, 1):
        @pl.when(has_side(way))
        def _():
            for piece in range(PIECES):
                q_copy(way, z, piece).wait_send()
                o_copy(way, z, piece).wait_send()
    qp_copy(z).wait_send()
    op_copy(z).wait_send()
    for k in range(1, Z):
        for way, src, there in sources(k):
            @pl.when(there)
            def _():
                qp_copy(src).wait_send()
                op_copy(src).wait_send()
                for piece in range(PIECES):
                    i_copy(0, src, piece).wait_send()
                    i_copy(1, src, piece).wait_send()
                    d_copy(src, piece).wait_send()

            @pl.when(there & has_side(way))
            def _():
                for piece in range(PIECES):
                    q_copy(way, src, piece).wait_send()
                    o_copy(way, src, piece).wait_send()
    for head in range(heads):
        for j in range(S):
            pl.when(j != s)(lambda: n_copy(head, j).wait_send())


def fused(S, Z, tokens, query_weight, key_weight, value_weight, output_weight, log_decay):
    rows, model = tokens.shape[1:]
    depth = query_weight.shape[0]
    heads = log_decay.shape[1]
    length = S * rows
    width = heads * (2 * DK + DV)
    oc = output_weight.shape[1] // S
    cosine, sine, swap = tables(length)
    vmem, anyplace = pl.BlockSpec(memory_space=pltpu.VMEM), pl.BlockSpec(memory_space=pl.ANY)
    dma = pltpu.SemaphoreType.DMA
    bf, f32 = jnp.bfloat16, jnp.float32
    out = pl.pallas_call(
        functools.partial(layer_kernel, S, Z),
        out_shape=jax.ShapeDtypeStruct((rows, output_weight.shape[1]), bf),
        in_specs=[pl.BlockSpec(memory_space=pltpu.SMEM)] + [vmem] * 3 + [anyplace] * 5,
        out_specs=vmem,
        scratch_shapes=[
            pltpu.VMEM((S, rows, model), bf),
            pltpu.VMEM((Z * CORES, depth, width), bf),
            pltpu.VMEM((Z * CORES, S, depth, oc), bf),
            pltpu.VMEM((length, width), f32),
            pltpu.VMEM((heads, length, length), f32),
            pltpu.VMEM((length, 2 * heads * DK), bf),
            pltpu.VMEM((length, heads * DV), bf),
            pltpu.VMEM((heads, S, rows, DV), bf),
            pltpu.VMEM((S, rows, heads * DV), bf),
            pltpu.VMEM((rows, S * oc), f32),
            dma((4 + S,)), dma((S,)), dma((S,)),
            dma((2, Z, PIECES)), dma((Z, PIECES)), dma((Z,)), dma((Z,)),
            dma((2, Z, PIECES)), dma((Z, PIECES)),
            dma((2, Z, PIECES)), dma((2, Z, PIECES)), dma((Z, PIECES)), dma((Z, PIECES)),
            dma((Z,)), dma((Z,)), dma((heads, S)), dma((heads, S)),
        ],
        compiler_params=pltpu.CompilerParams(
            collective_id=0, has_side_effects=True, vmem_limit_bytes=60 * 1024 * 1024
        ),
    )(log_decay, cosine, sine, swap, tokens[0], query_weight, key_weight, value_weight, output_weight)
    return out[None]


def solution(mesh):
    S, D = mesh.shape["sp"], mesh.shape["dp"]
    Z = D // CORES

    def layer(tokens, query_weight, key_weight, value_weight, output_weight, log_decay):
        rows = tokens.shape[1]
        depth = query_weight.shape[0]
        heads = log_decay.shape[1]
        fits = (
            S == 4 and D == CORES * Z and S * rows == BLOCK and (heads * DK) % 256 == 0
            and heads * DV == CORES * depth and rows % 128 == 0
        )
        args = (tokens, query_weight, key_weight, value_weight, output_weight, log_decay)
        return fused(S, Z, *args) if fits else shards(*args)

    placed = (
        P("dp", "sp", None),
        P("dp", None),
        P("dp", None),
        P("dp", None),
        P("dp", None),
        P(None, "sp"),
    )
    return jax.shard_map(
        layer, mesh=mesh, in_specs=placed, out_specs=P("dp", "sp", None), check_vma=False
    )
```

```python
import functools

import numpy as np
import jax
import jax.numpy as jnp
from jax import lax
from jax.experimental import pallas as pl
from jax.experimental.pallas import tpu as pltpu
from jax.sharding import PartitionSpec as P

HEADS = 16
DK = 64
DV = 128
BLOCK = 512


exact_precision = lax.Precision.HIGHEST


def rotate(values_part, positions):
    half_dim = values_part.shape[-1] // 2
    frequency = 10000.0 ** (-jnp.arange(half_dim, dtype=jnp.float32) / half_dim)
    angles = positions[:, None] * frequency[None, :]
    cosine = jnp.cos(angles)[:, None, :]
    sine_part = jnp.sin(angles)[:, None, :]
    first = values_part[..., :half_dim]
    second = values_part[..., half_dim:]
    return jnp.concatenate(
        [first * cosine - second * sine_part, first * sine_part + second * cosine], axis=-1
    )


def retain(query, key_rows, value_rows, log_rate):
    length, heads, key_dim = query.shape
    value_dim = value_rows.shape[-1]
    count = length // BLOCK
    offsets = jnp.arange(BLOCK, dtype=jnp.float32)
    distance = offsets[:, None] - offsets[None, :]
    decay_inner = jnp.where(
        distance[None] >= 0.0,
        jnp.exp(log_rate[:, None, None] * jnp.maximum(distance, 0.0)[None]),
        0.0,
    )
    decay_query = jnp.exp((offsets[:, None] + 1.0) * log_rate[None, :])[:, :, None]
    decay_key = jnp.exp((BLOCK - 1.0 - offsets)[:, None] * log_rate[None, :])[:, :, None]
    decay_block = jnp.exp(BLOCK * log_rate)[:, None, None]

    def blocks(array):
        return array.reshape(count, BLOCK, heads, array.shape[-1])

    def advance(state, inputs):
        query_block, key_block, value_block = inputs
        inner = (
            jnp.einsum("ihd,jhd->hij", query_block, key_block, preferred_element_type=jnp.float32)
            * decay_inner
        )
        result = jnp.einsum(
            "hij,jhv->ihv",
            inner.astype(jnp.bfloat16),
            value_block,
            preferred_element_type=jnp.float32,
        )
        query_wide = query_block.astype(jnp.float32) * decay_query
        result = result + jnp.einsum("ihd,hdv->ihv", query_wide, state, precision=exact_precision)
        key_wide = key_block.astype(jnp.float32) * decay_key
        state = state * decay_block + jnp.einsum(
            "jhd,jhv->hdv", key_wide, value_block.astype(jnp.float32), precision=exact_precision
        )
        return (state, result)

    initial = jnp.zeros((heads, key_dim, value_dim), jnp.float32)
    final_state, outputs = lax.scan(
        advance, initial, (blocks(query), blocks(key_rows), blocks(value_rows))
    )
    return outputs.reshape(length, heads, value_dim)


def mechanism(stacked, log_decay):
    length = stacked.shape[0]
    widened = stacked[..., : 2 * DK].astype(jnp.float32)
    positions = jnp.arange(length, dtype=jnp.float32)
    query = rotate(widened[..., :DK], positions).astype(jnp.bfloat16)
    key_rows = rotate(widened[..., DK : 2 * DK], positions).astype(jnp.bfloat16)
    value_rows = stacked[..., 2 * DK :]
    forward = retain(query, key_rows, value_rows, log_decay[0])
    backward = retain(
        jnp.flip(query, 0), jnp.flip(key_rows, 0), jnp.flip(value_rows, 0), log_decay[1]
    )
    combined = forward + jnp.flip(backward, 0)
    average = jnp.mean(combined, axis=-1, keepdims=True)
    centred = combined - average
    variance = jnp.mean(centred * centred, axis=-1, keepdims=True)
    return (centred * lax.rsqrt(variance + 1e-06)).astype(jnp.bfloat16)


def shards(tokens, query_weight, key_weight, value_weight, output_weight, log_decay):
    rows = tokens[0]
    row_count = rows.shape[0]
    local_heads = log_decay.shape[1]
    first_head = lax.axis_index("sp") * local_heads
    own_slices = jnp.concatenate(
        [
            lax.dynamic_slice_in_dim(query_weight, first_head * DK, local_heads * DK, 1),
            lax.dynamic_slice_in_dim(key_weight, first_head * DK, local_heads * DK, 1),
            lax.dynamic_slice_in_dim(value_weight, first_head * DV, local_heads * DV, 1),
        ],
        axis=1,
    )
    own_whole = lax.all_gather(own_slices, "dp", axis=0, tiled=True)
    piece = lax.all_gather(rows, "sp", axis=0, tiled=True)
    count = piece.shape[0]
    product = jnp.dot(piece, own_whole, preferred_element_type=jnp.float32).astype(jnp.bfloat16)
    query_part = product[:, : local_heads * DK].reshape(count, local_heads, DK)
    key_part = product[:, local_heads * DK : 2 * local_heads * DK].reshape(count, local_heads, DK)
    value_part = product[:, 2 * local_heads * DK :].reshape(count, local_heads, DV)
    gathered = jnp.concatenate([query_part, key_part, value_part], axis=2)
    normed = mechanism(gathered, log_decay)
    by_token = lax.all_to_all(normed, "sp", split_axis=0, concat_axis=1, tiled=True).reshape(
        row_count, HEADS * DV
    )
    mixed = jnp.dot(
        by_token,
        lax.all_gather(output_weight, "dp", axis=0, tiled=True),
        preferred_element_type=jnp.float32,
    )
    return mixed.astype(jnp.bfloat16)[None]


MESH = pl.DeviceIdType.MESH
CORES = 2
PIECES = 2


def tables(length):
    half = DK // 2
    frequency = (10000.0 ** (-np.arange(half) / half)).astype(np.float32)
    angles = (np.arange(length, dtype=np.float32)[:, None] * frequency[None, :]).astype(np.float64)
    cosine = np.tile(np.cos(angles), (1, 4)).astype(np.float32)
    sine = np.tile(np.sin(angles), (1, 4)).astype(np.float32)
    swap = np.zeros((2 * DK, 2 * DK), np.float32)
    for lane in range(2 * DK):
        if lane % DK < half:
            swap[lane + half, lane] = -1.0
        else:
            swap[lane - half, lane] = 1.0
    return jnp.asarray(cosine), jnp.asarray(sine), jnp.asarray(swap, jnp.bfloat16)


def layer_kernel(
    S, Z, rate_ref, cos_ref, sin_ref, swap_ref, x_ref, wq_ref, wk_ref, wv_ref, wo_ref, out_ref,
    tok, wqkv, wo, acc, decay, qk, val, nsend, nrm, oacc,
    lsem, tS, tR, qS, qR, qpS, qpR, oS, oR, iS, iR, dS, dR, opS, opR, nS, nR,
):
    s = lax.axis_index("sp")
    d = lax.axis_index("dp")
    z, c = d // CORES, d % CORES
    rows, model = x_ref.shape
    length = S * rows
    depth = wq_ref.shape[0]
    heads = rate_ref.shape[1]
    qc, vc = heads * DK, heads * DV
    oc = wo.shape[3]
    step_rows = depth // PIECES
    sx = s + 1 - 2 * (s % 2)
    sy = (s + 2) % 4
    sd = (sx + 2) % 4
    partner = {"dp": z * CORES + 1 - c}

    def remote(src, send, recv, device, dst=None):
        return pltpu.make_async_remote_copy(
            src_ref=src, dst_ref=src if dst is None else dst, send_sem=send, recv_sem=recv,
            device_id=device, device_id_type=MESH,
        )

    local = [
        pltpu.make_async_copy(wq_ref.at[:, pl.ds(pl.multiple_of(s * qc, qc), qc)], wqkv.at[d, :, pl.ds(0, qc)], lsem.at[0]),
        pltpu.make_async_copy(wk_ref.at[:, pl.ds(pl.multiple_of(s * qc, qc), qc)], wqkv.at[d, :, pl.ds(qc, qc)], lsem.at[1]),
        pltpu.make_async_copy(wv_ref.at[:, pl.ds(pl.multiple_of(s * vc, vc), vc)], wqkv.at[d, :, pl.ds(2 * qc, vc)], lsem.at[2]),
        pltpu.make_async_copy(x_ref, tok.at[s], lsem.at[3]),
    ] + [
        pltpu.make_async_copy(wo_ref.at[:, pl.ds(j * oc, oc)], wo.at[d, j], lsem.at[4 + j]) for j in range(S)
    ]
    for copy in local:
        copy.start()

    barrier = pltpu.get_barrier_semaphore()

    def greet(device):
        pl.semaphore_signal(barrier, inc=1, device_id=device, device_id_type=MESH)

    for other in range(1, S):
        greet({"sp": (s + other) % S})
    greet(partner)
    pl.when(z > 0)(lambda: greet({"dp": d - CORES}))
    pl.when(z < Z - 1)(lambda: greet({"dp": d + CORES}))
    inside = (z > 0) & (z < Z - 1)
    pl.when(inside)(lambda: pl.semaphore_wait(barrier, S + 2))
    pl.when(jnp.logical_not(inside))(lambda: pl.semaphore_wait(barrier, S + min(Z - 1, 1)))

    def side(way):
        return {"dp": d + CORES if way == 0 else d - CORES}

    def has_side(way):
        return z < Z - 1 if way == 0 else z > 0

    def q_copy(way, src, piece, to=None):
        ref = wqkv.at[src * CORES + c, pl.ds(piece * step_rows, step_rows)]
        return remote(ref, qS.at[way, src, piece], qR.at[src, piece], side(way if to is None else to))

    def o_piece(block, quarter, piece):
        return wo.at[block, quarter, pl.ds(piece * step_rows, step_rows)]

    def o_copy(way, src, piece, to=None):
        return remote(o_piece(src * CORES + c, s, piece), oS.at[way, src, piece], oR.at[src, piece], side(way if to is None else to))

    def qp_copy(src, mine=True):
        ref = wqkv.at[src * CORES + (c if mine else 1 - c)]
        return remote(ref, qpS.at[src], qpR.at[src], partner)

    def op_copy(src, mine=True):
        ref = wo.at[src * CORES + (c if mine else 1 - c)]
        return remote(ref, opS.at[src], opR.at[src], partner)

    def i_copy(axis, src, piece, mine=True):
        to = sx if axis == 0 else sy
        return remote(o_piece(src * CORES + c, s if mine else to, piece), iS.at[axis, src, piece], iR.at[axis, src, piece], {"sp": to})

    def d_copy(src, piece, mine=True):
        first = piece < PIECES // 2
        to = sy if first else sx
        quarter = (sx if first else sy) if mine else sd
        return remote(o_piece(src * CORES + c, quarter, piece), dS.at[src, piece], dR.at[src, piece], {"sp": to})

    def t_copy(other):
        to = (s + other) % S
        return remote(tok.at[s], tS.at[other], tR.at[other], {"sp": to})

    def t_wait(other):
        frm = (s + S - other) % S
        remote(tok.at[frm], tS.at[other], tR.at[other], {"sp": frm}).wait_recv()

    def n_copy(head, j):
        return remote(
            nsend.at[head, j], nS.at[head, j], nR.at[head, s], {"sp": j},
            dst=nrm.at[s, :, pl.ds(head * DV, DV)],
        )

    def n_wait(head, j):
        remote(nsend.at[head, j], nS.at[head, j], nR.at[head, j], {"sp": j}, dst=nrm.at[j, :, pl.ds(head * DV, DV)]).wait_recv()

    def each(count, fn):
        for piece in range(count):
            fn(piece)

    def own_o(way):
        each(PIECES, lambda piece: o_copy(way, z, piece).start())

    for copy in local[:3]:
        copy.wait()
    for way in (0, 1):
        pl.when(has_side(way))(lambda way=way: each(PIECES, lambda piece: q_copy(way, z, piece).start()))
    local[3].wait()
    for other in range(1, S):
        t_copy(other).start()
    qp_copy(z).start()
    for copy in local[4:]:
        copy.wait()
    for way in (0, 1):
        pl.when(has_side(way))(lambda way=way: own_o(way))
    op_copy(z).start()

    for head in range(heads):
        fast, slow = rate_ref[0, head], rate_ref[1, head]

        @pl.loop(0, S)
        def _(j):
            at = lax.broadcasted_iota(jnp.int32, (rows, length), 0) + j * rows
            gap = (at - lax.broadcasted_iota(jnp.int32, (rows, length), 1)).astype(jnp.float32)
            weight = jnp.exp(jnp.where(gap >= 0.0, gap * fast, gap * (-slow)))
            decay[head, pl.ds(pl.multiple_of(j * rows, rows), rows), :] = jnp.where(gap == 0.0, 2.0, weight)

    width = 2 * qc + vc
    tile = 256

    def project(src, first):
        qp_copy(src, mine=False).wait_recv()
        wide = CORES * depth
        cols = pl.ds(pl.multiple_of(src * wide, wide), wide)

        @pl.loop(0, width // tile)
        def _(n):
            at = pl.ds(pl.multiple_of(n * tile, tile), tile)
            part = jnp.dot(
                tok[:, :, cols].reshape(length, wide),
                wqkv[pl.ds(src * CORES, CORES), :, at].reshape(wide, tile),
                preferred_element_type=jnp.float32,
            )
            if first:
                acc[:, at] = part
            else:
                acc[:, at] += part

    def sources(k):
        return ((0, z - k, z - k >= 0), (1, z + k, z + k < Z))

    def q_step(k):
        for way, src, there in sources(k):
            @pl.when(there)
            def _():
                for piece in range(PIECES):
                    q_copy(way, src, piece, 1 - way).wait_recv()
                    pl.when(has_side(way))(lambda: q_copy(way, src, piece).start())
                qp_copy(src).start()

    def o_step(k):
        for way, src, there in sources(k):
            @pl.when(there)
            def _():
                for piece in range(PIECES):
                    o_copy(way, src, piece, 1 - way).wait_recv()
                    pl.when(has_side(way))(lambda: o_copy(way, src, piece).start())
                for piece in range(PIECES):
                    i_copy(0, src, piece).start()
                    i_copy(1, src, PIECES - 1 - piece).start()

    def o_relay(k):
        for way, src, there in sources(k):
            @pl.when(there)
            def _():
                for near in range(PIECES // 2):
                    for axis, piece in ((0, near), (1, PIECES - 1 - near)):
                        i_copy(axis, src, piece, mine=False).wait_recv()
                        d_copy(src, piece).start()

    def o_share(k):
        for way, src, there in sources(k):
            @pl.when(there)
            def _():
                for near in range(PIECES // 2):
                    i_copy(1, src, near, mine=False).wait_recv()
                    i_copy(0, src, PIECES - 1 - near, mine=False).wait_recv()
                for piece in range(PIECES):
                    d_copy(src, piece, mine=False).wait_recv()
                op_copy(src).start()

    def project_step(k):
        for way, src, there in sources(k):
            pl.when(there)(lambda: project(src, False))

    q_step(1)
    o_step(1)
    for other in range(1, S):
        t_wait(other)
    project(z, True)
    project_step(1)
    q_step(2)
    o_step(2)
    o_relay(1)
    project_step(2)
    q_step(3)
    project_step(3)

    for pair in range(qc // (2 * DK)):
        for part in range(2):
            at = pl.ds(part * qc + pair * 2 * DK, 2 * DK)
            flat = acc[:, at].astype(jnp.bfloat16)
            turned = jnp.dot(flat, swap_ref[...], preferred_element_type=jnp.float32)
            qk[:, at] = (flat.astype(jnp.float32) * cos_ref[...] + turned * sin_ref[...]).astype(jnp.bfloat16)
    val[...] = acc[:, 2 * qc :].astype(jnp.bfloat16)

    def retain_head(head):
        pair = head // 2
        lane = lax.broadcasted_iota(jnp.int32, (rows, 2 * DK), 1)
        mine = (lane // DK) == (head % 2)
        for j in range(S):
            here = slice(j * rows, (j + 1) * rows)
            query = qk[here, pair * 2 * DK : (pair + 1) * 2 * DK]
            query = jnp.where(mine, query.astype(jnp.float32), 0.0).astype(jnp.bfloat16)
            scores = lax.dot_general(
                query, qk[:, qc + pair * 2 * DK : qc + (pair + 1) * 2 * DK],
                (((1,), (1,)), ((), ())), preferred_element_type=jnp.float32,
            )
            scores = (scores * decay[head, here, :]).astype(jnp.bfloat16)
            ret = jnp.dot(scores, val[:, head * DV : (head + 1) * DV], preferred_element_type=jnp.float32)
            centred = ret - jnp.mean(ret, axis=-1, keepdims=True)
            variance = jnp.mean(centred * centred, axis=-1, keepdims=True)
            normed = (centred * lax.rsqrt(variance + 1e-06)).astype(jnp.bfloat16)
            nsend[head, j] = normed

            @pl.when(j == s)
            def _():
                nrm[s, :, head * DV : (head + 1) * DV] = normed

            @pl.when(j != s)
            def _():
                n_copy(head, j).start()

    def finish(src, first):
        op_copy(src, mine=False).wait_recv()

        @pl.loop(0, S)
        def _(j):
            at = pl.ds(pl.multiple_of(j * oc, oc), oc)
            part = jnp.dot(
                nrm[src], wo[pl.ds(src * CORES, CORES), j].reshape(CORES * depth, oc),
                preferred_element_type=jnp.float32,
            )
            if first:
                oacc[:, at] = part
            else:
                oacc[:, at] += part

    def finish_step(k):
        for way, src, there in sources(k):
            pl.when(there)(lambda: finish(src, False))

    for head in range(heads):
        retain_head(head)
        if head == 0:
            o_relay(2)
        if head == heads - 2:
            o_step(3)
    o_share(1)
    o_relay(3)
    for j in range(S):
        @pl.when(j != s)
        def _():
            for head in range(heads):
                n_wait(head, j)
    finish(z, True)
    finish_step(1)
    o_share(2)
    o_share(3)
    finish_step(2)
    finish_step(3)
    out_ref[...] = oacc[...].astype(out_ref.dtype)

    for other in range(1, S):
        t_copy(other).wait_send()
    for way in (0, 1):
        @pl.when(has_side(way))
        def _():
            for piece in range(PIECES):
                q_copy(way, z, piece).wait_send()
                o_copy(way, z, piece).wait_send()
    qp_copy(z).wait_send()
    op_copy(z).wait_send()
    for k in range(1, Z):
        for way, src, there in sources(k):
            @pl.when(there)
            def _():
                qp_copy(src).wait_send()
                op_copy(src).wait_send()
                for piece in range(PIECES):
                    i_copy(0, src, piece).wait_send()
                    i_copy(1, src, piece).wait_send()
                    d_copy(src, piece).wait_send()

            @pl.when(there & has_side(way))
            def _():
                for piece in range(PIECES):
                    q_copy(way, src, piece).wait_send()
                    o_copy(way, src, piece).wait_send()
    for head in range(heads):
        for j in range(S):
            pl.when(j != s)(lambda: n_copy(head, j).wait_send())


def fused(S, Z, tokens, query_weight, key_weight, value_weight, output_weight, log_decay):
    rows, model = tokens.shape[1:]
    depth = query_weight.shape[0]
    heads = log_decay.shape[1]
    length = S * rows
    width = heads * (2 * DK + DV)
    oc = output_weight.shape[1] // S
    cosine, sine, swap = tables(length)
    vmem, anyplace = pl.BlockSpec(memory_space=pltpu.VMEM), pl.BlockSpec(memory_space=pl.ANY)
    dma = pltpu.SemaphoreType.DMA
    bf, f32 = jnp.bfloat16, jnp.float32
    out = pl.pallas_call(
        functools.partial(layer_kernel, S, Z),
        out_shape=jax.ShapeDtypeStruct((rows, output_weight.shape[1]), bf),
        in_specs=[pl.BlockSpec(memory_space=pltpu.SMEM)] + [vmem] * 3 + [anyplace] * 5,
        out_specs=vmem,
        scratch_shapes=[
            pltpu.VMEM((S, rows, model), bf),
            pltpu.VMEM((Z * CORES, depth, width), bf),
            pltpu.VMEM((Z * CORES, S, depth, oc), bf),
            pltpu.VMEM((length, width), f32),
            pltpu.VMEM((heads, length, length), f32),
            pltpu.VMEM((length, 2 * heads * DK), bf),
            pltpu.VMEM((length, heads * DV), bf),
            pltpu.VMEM((heads, S, rows, DV), bf),
            pltpu.VMEM((S, rows, heads * DV), bf),
            pltpu.VMEM((rows, S * oc), f32),
            dma((4 + S,)), dma((S,)), dma((S,)),
            dma((2, Z, PIECES)), dma((Z, PIECES)), dma((Z,)), dma((Z,)),
            dma((2, Z, PIECES)), dma((Z, PIECES)),
            dma((2, Z, PIECES)), dma((2, Z, PIECES)), dma((Z, PIECES)), dma((Z, PIECES)),
            dma((Z,)), dma((Z,)), dma((heads, S)), dma((heads, S)),
        ],
        compiler_params=pltpu.CompilerParams(
            collective_id=0, has_side_effects=True, vmem_limit_bytes=60 * 1024 * 1024
        ),
    )(log_decay, cosine, sine, swap, tokens[0], query_weight, key_weight, value_weight, output_weight)
    return out[None]


def solution(mesh):
    S, D = mesh.shape["sp"], mesh.shape["dp"]
    Z = D // CORES

    def layer(tokens, query_weight, key_weight, value_weight, output_weight, log_decay):
        rows = tokens.shape[1]
        depth = query_weight.shape[0]
        heads = log_decay.shape[1]
        fits = (
            S == 4 and D == CORES * Z and S * rows == BLOCK and (heads * DK) % 256 == 0
            and heads * DV == CORES * depth and rows % 128 == 0
        )
        args = (tokens, query_weight, key_weight, value_weight, output_weight, log_decay)
        return fused(S, Z, *args) if fits else shards(*args)

    placed = (
        P("dp", "sp", None),
        P("dp", None),
        P("dp", None),
        P("dp", None),
        P("dp", None),
        P(None, "sp"),
    )
    return jax.shard_map(
        layer, mesh=mesh, in_specs=placed, out_specs=P("dp", "sp", None), check_vma=False
    )
```
